32 devices in a mesh: fs: 16 (over z, y, x), tp: 2 (over core).
Axes of the slice: x: 2, y: 2, z: 4, core: 2. Of those that a mesh axis runs over, the one named last changes fastest.
Arguments:
- tokens: bfloat16 [8192, 2048], P('fs'), may hold values from -6 to 6
- mixer_gain: float32 [2048], replicated, may hold values from 0.1 to 1.9
- w_query: bfloat16 [2048, 1024], P('fs', 'tp'), may hold values from -0.125 to 0.125
- w_key: bfloat16 [2048, 1024], P('fs', 'tp'), may hold values from -0.125 to 0.125
- w_value: bfloat16 [2048, 2048], P('fs', 'tp'), may hold values from -0.125 to 0.125
- gate_down: bfloat16 [2048, 32], replicated, may hold values from -0.125 to 0.125
- gate_up: bfloat16 [32, 1024], P(None, 'tp'), may hold values from -1 to 1
- decay_bias: float32 [1024], P('tp'), may hold values from -1 to 6
- decay_shift: float32 [8192, 8], P('fs', 'tp'), may hold values from -0.71 to 0, as said below
- head_gain: float32 [2048], P('tp'), may hold values from 0.1 to 1.9
- w_out: bfloat16 [2048, 2048], P('fs', 'tp'), may hold values from -0.125 to 0.125
- mlp_gain: float32 [2048], replicated, may hold values from 0.1 to 1.9
- mlp_up: bfloat16 [2048, 8192], P('fs', 'tp'), may hold values from -0.125 to 0.125
- mlp_down: bfloat16 [2048, 8192], P('fs', 'tp'), may hold values from -0.0625 to 0.0625
Outputs:
- layer_out: bfloat16 [8192, 2048], P('fs')
The draws below stay inside these ranges and needn't reach their ends.
Inputs may be any that keep to these rules, and one draw needn't show every extreme that they name: `decay_shift`: never positive.
All inputs are finite; a program needn't handle non-finite values.
Results may differ from the reference program's by a relative error of at most 0.022.
Values may be sent and summed in bfloat16 or wider, within the bound.
No kernel may reach another device: no remote copies, remote signals or barrier semaphores. Data moves between devices by JAX's collectives and lax.ppermute only.
A program may use at most 128 MiB of HBM per device.

```python
import math
import jax
import jax.numpy as jnp
from jax import lax

D = 2048
ATTENTION_HEADS = 8
HEAD_K = 128
FF = 8192
RANK = 32
BLOCK_TOKENS = 64
SEQUENCE_LENGTH = 512
DK = 1024
DV = 2048
TOKENS = 8192
N_TP = 2


def draw_decay_bias(key, part):
    return jax.random.uniform(key, (ATTENTION_HEADS * HEAD_K,), jnp.float32, -1.0, 5.0)


def draw_decay_shift(key, part):
    decay_rate_key, jitter_random_key, spike_random_key, layer_depth_key = jax.random.split(jax.random.fold_in(key, 11), 4)
    every_block = TOKENS // BLOCK_TOKENS
    decay_rates = jnp.exp(jax.random.uniform(decay_rate_key, (every_block, 1, ATTENTION_HEADS), jnp.float32, math.log(0.0005), math.log(0.004)))
    random_jitter = jax.random.uniform(jitter_random_key, (every_block, BLOCK_TOKENS, ATTENTION_HEADS), jnp.float32, 0.0, 2.0)
    spike_values = jax.random.randint(spike_random_key, (every_block, BLOCK_TOKENS, ATTENTION_HEADS), 0, SEQUENCE_LENGTH) < 2
    layer_depth = jnp.log(jax.random.uniform(layer_depth_key, (every_block, BLOCK_TOKENS, ATTENTION_HEADS), jnp.float32, 0.5, 0.8))
    offset_amount = -decay_rates * random_jitter + jnp.where(spike_values, layer_depth, 0.0)
    return offset_amount.reshape(TOKENS, ATTENTION_HEADS).astype(jnp.float32)


def block_scale(stream_key, shape, cuts, least, largest):
    factor_of = 1.0
    for axis_at, blocks in cuts:
        steps = jax.random.uniform(jax.random.fold_in(jax.random.fold_in(stream_key, 6), axis_at), (blocks,), jnp.float32, least / len(cuts), largest / len(cuts))
        factor_of = factor_of * jnp.repeat(jnp.exp(steps), shape[axis_at] // blocks).reshape((-1,) + (1,) * (len(shape) - 1 - axis_at))
    return factor_of


def centred(key, extent, spread, bound, cuts=(), kind=jnp.bfloat16):
    result = jax.random.normal(key, extent, jnp.float32) * spread
    if len(cuts) > 0:
        result = block_scale(key, extent, cuts, -0.22, 0.18) * result
    return jnp.clip(result, min=-bound, max=bound).astype(kind)


def setup_inputs(seed: int = 0) -> dict:
    key_of = jax.random.split(jax.random.key(seed), 15)
    return {
        "tokens": centred(key_of[0], (TOKENS, D), 1.0, 6.0, ((0, 16),)),
        "mixer_gain": jnp.clip(1.0 + 0.18 * jax.random.normal(key_of[1], (D,), jnp.float32), 0.1, 1.9),
        "w_query": centred(key_of[2], (D, DK), D ** -0.5, 0.125, ((0, 16), (1, 2))),
        "w_key": centred(key_of[3], (D, DK), D ** -0.5, 0.125, ((0, 16), (1, 2))),
        "w_value": centred(key_of[4], (D, DV), D ** -0.5, 0.125, ((0, 16), (1, 2))),
        "gate_down": centred(key_of[5], (D, RANK), D ** -0.5, 0.125),
        "gate_up": centred(key_of[6], (RANK, DK), RANK ** -0.5, 1.0, ((1, 2),)),
        "decay_bias": draw_decay_bias(jax.random.fold_in(key_of[14], 71), 0),
        "decay_shift": draw_decay_shift(jax.random.fold_in(key_of[14], 71), 0),
        "head_gain": jnp.clip(1.0 + 0.18 * jax.random.normal(key_of[9], (DV,), jnp.float32), 0.1, 1.9),
        "w_out": centred(key_of[10], (D, DV), DV ** -0.5, 0.125, ((0, 16), (1, 2))),
        "mlp_gain": jnp.clip(1.0 + 0.18 * jax.random.normal(key_of[11], (D,), jnp.float32), 0.1, 1.9),
        "mlp_up": centred(key_of[12], (D, FF), D ** -0.5, 0.125, ((0, 16), (1, 2))),
        "mlp_down": centred(key_of[13], (D, FF), FF ** -0.5, 0.0625, ((0, 16), (1, 2))),
    }


epsilon = 1e-06
decay_temper = 16.0
highest = lax.Precision.HIGHEST

def rms_rows(row_block, row_gain):
    values = row_block.astype(jnp.float32)
    inverse = lax.rsqrt(lax.optimization_barrier(jnp.mean(values * values, axis=-1, keepdims=True)) + epsilon)
    return (values * inverse * row_gain).astype(jnp.bfloat16)

def one_direction(queries, keyed, valued, log_decay):
    cumulative = jnp.cumsum(log_decay, axis=2)
    block_end = cumulative[:, :, -1:, :]
    q_decayed = queries * jnp.exp(cumulative)
    k_decayed = keyed * jnp.exp(-cumulative)
    block_len = queries.shape[2]
    lower_mask = jnp.tril(jnp.ones((block_len, block_len), dtype=bool))
    scores = jnp.where(lower_mask, jnp.einsum('nhtd,nhsd->nhts', q_decayed, k_decayed, precision=highest), 0.0)
    within = jnp.einsum('nhts,nhsv->nhtv', scores, valued, precision=highest)
    k_tail = keyed * jnp.exp(block_end - cumulative)
    contrib = jnp.einsum('nhsd,nhsv->nhdv', k_tail, valued, precision=highest)
    fading = jnp.exp(block_end[:, :, 0, :])

    def carry_step(state_now, pieces):
        addend, factor = pieces
        return (factor[..., None] * state_now + addend, state_now)
    start_state = jnp.zeros(contrib.shape[1:], jnp.float32)
    _, before = lax.scan(carry_step, start_state, (contrib, fading))
    carried = jnp.einsum('nhtd,nhdv->nhtv', q_decayed, before, precision=highest)
    return within + carried

def mix_heads(queries, keyed, valued, gate_low, gate_up, decay_bias, seq_shift, head_gain):
    length = queries.shape[0]
    head_count = seq_shift.shape[1]
    head_k = queries.shape[1] // head_count
    head_v = valued.shape[1] // head_count
    blocks = length // BLOCK_TOKENS
    gate_pre = jnp.dot(gate_low, gate_up, preferred_element_type=jnp.float32) + decay_bias
    log_decay = jax.nn.log_sigmoid(gate_pre) / decay_temper
    log_decay = log_decay.reshape(length, head_count, head_k) + seq_shift[:, :, None]
    query_f = queries.astype(jnp.float32).reshape(length, head_count, head_k) * head_k ** (-0.5)
    key_f = keyed.astype(jnp.float32).reshape(length, head_count, head_k)
    value_f = valued.astype(jnp.float32).reshape(length, head_count, head_v)

    def to_blocks(tensor):
        return tensor.reshape(blocks, BLOCK_TOKENS, head_count, tensor.shape[-1]).transpose(0, 2, 1, 3)

    def from_blocks(tensor):
        return tensor.transpose(0, 2, 1, 3).reshape(length, head_count, tensor.shape[-1])
    forward = from_blocks(one_direction(to_blocks(query_f), to_blocks(key_f), to_blocks(value_f), to_blocks(log_decay)))
    backward = from_blocks(one_direction(to_blocks(jnp.flip(query_f, 0)), to_blocks(jnp.flip(key_f, 0)), to_blocks(jnp.flip(value_f, 0)), to_blocks(jnp.flip(log_decay, 0))))
    outcome = forward + jnp.flip(backward, 0)
    inverse = lax.rsqrt(lax.optimization_barrier(jnp.mean(outcome * outcome, axis=-1, keepdims=True)) + epsilon)
    normed = outcome * inverse * head_gain.reshape(head_count, head_v)
    return normed.reshape(length, head_count * head_v).astype(jnp.bfloat16)

def group_sum(left, right):
    left_groups = left.astype(jnp.float32).reshape(left.shape[0], N_TP, -1)
    right_groups = right.astype(jnp.float32).reshape(right.shape[0], N_TP, -1)
    terms = jnp.einsum('lgc,dgc->gld', left_groups, right_groups)
    rounded = lax.optimization_barrier(terms.astype(jnp.bfloat16))
    return lax.optimization_barrier(jnp.sum(rounded.astype(jnp.float32), axis=0))

def reference(tokens, mixer_gain, w_query, w_key, w_value, gate_down, gate_up, decay_bias, decay_shift, head_gain, w_out, mlp_gain, mlp_up, mlp_down):
    model_width = tokens.shape[1]

    def one_sequence(pieces):
        seq_rows, seq_shift = pieces
        normed = rms_rows(seq_rows, mixer_gain)
        queries = jnp.dot(normed, w_query, preferred_element_type=jnp.float32).astype(jnp.bfloat16)
        keyed = jnp.dot(normed, w_key, preferred_element_type=jnp.float32).astype(jnp.bfloat16)
        valued = jnp.dot(normed, w_value, preferred_element_type=jnp.float32).astype(jnp.bfloat16)
        gate_low = jnp.dot(normed, gate_down, preferred_element_type=jnp.float32).astype(jnp.bfloat16)
        mixer_out = mix_heads(queries, keyed, valued, gate_low, gate_up, decay_bias, seq_shift, head_gain)
        after_mixer = (seq_rows.astype(jnp.float32) + group_sum(mixer_out, w_out)).astype(jnp.bfloat16)
        normed_two = rms_rows(after_mixer, mlp_gain)
        pre_act = jnp.dot(normed_two, mlp_up, preferred_element_type=jnp.float32)
        hidden = jnp.square(jax.nn.relu(pre_act)).astype(jnp.bfloat16)
        return (after_mixer.astype(jnp.float32) + group_sum(hidden, mlp_down)).astype(jnp.bfloat16)
    sequences = tokens.reshape(-1, SEQUENCE_LENGTH, model_width)
    shifts = decay_shift.reshape(-1, SEQUENCE_LENGTH, decay_shift.shape[1])
    return lax.map(one_sequence, (sequences, shifts)).reshape(tokens.shape)
```

```python
import functools

import jax
import jax.numpy as jnp
from jax import lax
from jax.experimental import pallas as pl
from jax.experimental.pallas import tpu as pltpu
from jax.sharding import PartitionSpec as P


BLOCK_TOKENS = 64
SPAN = 2 * BLOCK_TOKENS

epsilon = 1e-06
decay_temper = 16.0
highest = lax.Precision.HIGHEST
f32 = jnp.float32
bf16 = jnp.bfloat16

NT = (((1,), (1,)), ((), ()))
TN = (((0,), (0,)), ((), ()))


def rms_rows(row_block, row_gain):
    values = row_block.astype(f32)
    inverse = lax.rsqrt(jnp.mean(values * values, axis=-1, keepdims=True) + epsilon)
    return (values * inverse * row_gain).astype(bf16)


def attention_kernel(
    rows_each, place_ref, q_ref, k_ref, v_ref, low_ref, up_ref, bias_ref, shift_ref, gain_ref, out_ref, acc_ref
):
    head = pl.program_id(0)
    length, head_k = q_ref.shape
    head_v = v_ref.shape[1]
    spans = length // SPAN
    shifts = shift_ref[...]
    heads_at = lax.broadcasted_iota(jnp.int32, shifts.shape, 1)
    shift = jnp.sum(jnp.where(heads_at == head, shifts, 0.0), axis=1, keepdims=True)
    pre = jnp.dot(low_ref[...], up_ref[...], preferred_element_type=f32) + bias_ref[...]
    log_sig = jnp.minimum(pre, 0.0) - jnp.log1p(jnp.exp(-jnp.abs(pre)))
    log_decay = log_sig / decay_temper + shift
    row_at = lax.broadcasted_iota(jnp.int32, (SPAN, SPAN), 0)
    col_at = lax.broadcasted_iota(jnp.int32, (SPAN, SPAN), 1)
    lower = row_at >= col_at
    upper = row_at <= col_at
    ones_lower = lower.astype(f32)
    scale = head_k ** (-0.5)
    kept = []
    state = jnp.zeros((head_v, head_k), f32)
    for at in range(spans):
        rows = pl.ds(at * SPAN, SPAN)
        decay = log_decay[at * SPAN : (at + 1) * SPAN]
        upto = jnp.dot(ones_lower, decay, precision=highest, preferred_element_type=f32)
        before = upto - decay
        middle = upto[BLOCK_TOKENS - 1 : BLOCK_TOKENS]
        total = upto[SPAN - 1 : SPAN]
        q = q_ref[rows, :].astype(f32) * scale
        k = k_ref[rows, :].astype(f32)
        v = v_ref[rows, :]
        q_fwd = (q * jnp.exp(upto - middle)).astype(bf16)
        k_fwd = (k * jnp.exp(middle - upto)).astype(bf16)
        q_bwd = (q * jnp.exp(middle - before)).astype(bf16)
        k_bwd = (k * jnp.exp(before - middle)).astype(bf16)
        fwd = lax.dot_general(q_fwd, k_fwd, NT, preferred_element_type=f32)
        bwd = lax.dot_general(q_bwd, k_bwd, NT, preferred_element_type=f32)
        scores = jnp.where(lower, fwd, 0.0) + jnp.where(upper, bwd, 0.0)
        result = jnp.dot(scores.astype(bf16), v, preferred_element_type=f32)
        if at > 0:
            q_in = (q * jnp.exp(upto)).astype(bf16)
            result += lax.dot_general(q_in, state.astype(bf16), NT, preferred_element_type=f32)
        acc_ref[rows, :] = result
        if at < spans - 1:
            k_tail = (k * jnp.exp(total - upto)).astype(bf16)
            added = lax.dot_general(v, k_tail, TN, preferred_element_type=f32)
            state = state * jnp.exp(total) + added
        kept.append((before, total))
    state = jnp.zeros((head_v, head_k), f32)
    place = place_ref[0]
    step = min(rows_each, SPAN)
    for at in reversed(range(spans)):
        rows = pl.ds(at * SPAN, SPAN)
        before, total = kept[at]
        result = acc_ref[rows, :]
        if at < spans - 1:
            q = q_ref[rows, :].astype(f32) * scale
            q_out = (q * jnp.exp(total - before)).astype(bf16)
            result += lax.dot_general(q_out, state.astype(bf16), NT, preferred_element_type=f32)
        if at > 0:
            k_head = (k_ref[rows, :].astype(f32) * jnp.exp(before)).astype(bf16)
            added = lax.dot_general(v_ref[rows, :], k_head, TN, preferred_element_type=f32)
            state = state * jnp.exp(total) + added
        inverse = lax.rsqrt(jnp.mean(result * result, axis=-1, keepdims=True) + epsilon)
        normed = (result * inverse * gain_ref[...]).astype(bf16)
        for part in range(SPAN // step):
            first = at * SPAN + part * step
            slot = (first // rows_each) ^ place
            target = pl.multiple_of(slot * rows_each + first % rows_each, step)
            out_ref[pl.ds(target, step), :] = normed[part * step : (part + 1) * step]


def attention(queries, keyed, valued, gate_low, gate_up, decay_bias, shift, head_gain, place, n_tp):
    length = queries.shape[0]
    heads = shift.shape[1]
    head_k = queries.shape[1] // heads
    head_v = valued.shape[1] // heads
    rank = gate_low.shape[1]
    whole = lambda h, *_: (0, 0)
    column = lambda h, *_: (0, h)
    return pl.pallas_call(
        functools.partial(attention_kernel, length // n_tp),
        grid_spec=pltpu.PrefetchScalarGridSpec(
            num_scalar_prefetch=1,
            grid=(heads,),
            in_specs=[
                pl.BlockSpec((length, head_k), column),
                pl.BlockSpec((length, head_k), column),
                pl.BlockSpec((length, head_v), column),
                pl.BlockSpec((length, rank), whole),
                pl.BlockSpec((rank, head_k), column),
                pl.BlockSpec((1, head_k), column),
                pl.BlockSpec((length, heads), whole),
                pl.BlockSpec((1, head_v), column),
            ],
            out_specs=pl.BlockSpec((length, head_v), column),
            scratch_shapes=[pltpu.VMEM((length, head_v), f32)],
        ),
        out_shape=jax.ShapeDtypeStruct((length, heads * head_v), bf16),
        cost_estimate=pl.CostEstimate(
            flops=8_000_000_000, bytes_accessed=4_000_000, transcendentals=3_000_000
        ),
    )(
        place.reshape(1),
        queries,
        keyed,
        valued,
        gate_low,
        gate_up,
        decay_bias.reshape(1, -1),
        shift,
        head_gain.reshape(1, -1),
    )


def copy_kernel(index_ref, in_ref, out_ref):
    out_ref[...] = in_ref[...]


def pick_columns(matrix, sources):
    rows, width = matrix.shape
    count = sources.shape[0]
    block = width // count
    if block % 128:
        return matrix.reshape(rows, count, block)[:, sources, :].reshape(rows, width)
    return pl.pallas_call(
        copy_kernel,
        grid_spec=pltpu.PrefetchScalarGridSpec(
            num_scalar_prefetch=1,
            grid=(count,),
            in_specs=[pl.BlockSpec((rows, block), lambda i, index: (0, index[i]))],
            out_specs=pl.BlockSpec((rows, block), lambda i, index: (0, i)),
        ),
        out_shape=jax.ShapeDtypeStruct(matrix.shape, matrix.dtype),
    )(sources, matrix)


def reorder(matrix, have, want):
    block = matrix.shape[1] // len(have)
    at = [have.index(mask) for mask in want]
    return jnp.concatenate([matrix[:, i * block : (i + 1) * block] for i in at], axis=1)


def fused_dot(left, pieces):
    total, start = None, 0
    for piece in pieces:
        part = jnp.dot(
            left[:, start : start + piece.shape[0]], piece, preferred_element_type=f32
        )
        total = part if total is None else total + part
        start += piece.shape[0]
    return total


def per_device(
    n_fs,
    n_tp,
    tokens,
    mixer_gain,
    w_query,
    w_key,
    w_value,
    gate_down,
    gate_up,
    decay_bias,
    decay_shift,
    head_gain,
    w_out,
    mlp_gain,
    mlp_up,
    mlp_down,
):
    me = lax.axis_index("fs")
    core = lax.axis_index("tp")
    length, width = tokens.shape
    own_rows = length // n_tp
    high = []
    bit = n_fs // 2
    while bit >= 4:
        high.append(bit)
        bit //= 2

    def swap(value, mask):
        return lax.ppermute(value, "fs", [(i, i ^ mask) for i in range(n_fs)])

    def swap_tp(value, mask):
        return lax.ppermute(value, "tp", [(i, i ^ mask) for i in range(n_tp)])

    def double(held, masks, bits):
        for bit in bits:
            held = jnp.concatenate([held, swap(held, bit)], axis=0)
            masks = masks + [m ^ bit for m in masks]
        return held, masks

    def spread(held, masks):
        half = held.shape[0] // 2
        from_x, from_y = swap(held, 1), swap(held, 2)
        corner_a = swap(from_x[:half], 2)
        corner_b = swap(from_y[half:], 1)
        masks = masks + [m ^ 1 for m in masks] + [m ^ 2 for m in masks] + [m ^ 3 for m in masks]
        return [held, from_x, from_y, corner_a, corner_b], masks

    def gather_outer(shard):
        held, masks = double(shard, [0], high)
        return spread(held, masks)

    def gather_inner(shard):
        pieces, masks = spread(shard, [0])
        held, masks = double(jnp.concatenate(pieces, axis=0), masks, high)
        return [held], masks

    key_pieces, order_a = gather_outer(w_key)
    query_pieces, order_c = gather_inner(w_query)
    value_pieces, _ = gather_outer(w_value)

    group = [0, 1, 4, 5]
    quarter = (me & 1) + ((me >> 2) & 1) * 2

    def to_group(shard):
        cut = shard.shape[1] // len(group)
        parts = shard.reshape(shard.shape[0], len(group), cut)
        held = []
        for slot, mask in enumerate(group):
            part = lax.dynamic_index_in_dim(parts, quarter ^ slot, axis=1, keepdims=False)
            held.append(part if mask == 0 else swap(part, mask))
        return jnp.concatenate(held, axis=0)

    def gather_mlp(shard):
        held, masks = double(to_group(shard), group, [b for b in high if b != 4])
        return [held, swap(held, 2)], masks + [m ^ 2 for m in masks]

    up_pieces, order_m = gather_mlp(mlp_up)
    out_pieces, order_o = gather_outer(w_out)
    down_pieces, _ = gather_mlp(mlp_down)

    normed = rms_rows(tokens, mixer_gain)
    gate_low = jnp.dot(normed, gate_down, preferred_element_type=f32).astype(bf16)
    normed_a = pick_columns(normed, me ^ jnp.array(order_a, jnp.int32))
    normed_c = reorder(normed_a, order_a, order_c)
    tokens_own = lax.dynamic_slice_in_dim(tokens, core * own_rows, own_rows, axis=0)
    tokens_own = pick_columns(tokens_own, me ^ jnp.array(order_m, jnp.int32))
    gain_m = mlp_gain.reshape(n_fs, -1)[me ^ jnp.array(order_m, jnp.int32)].reshape(1, width)

    keyed = fused_dot(normed_a, key_pieces).astype(bf16)
    queries = fused_dot(normed_c, query_pieces).astype(bf16)
    valued = fused_dot(normed_a, value_pieces).astype(bf16)

    mixed = attention(
        queries, keyed, valued, gate_low, gate_up, decay_bias, decay_shift, head_gain, core, n_tp
    )

    def project(rows, pieces):
        return jnp.concatenate(
            [
                lax.dot_general(rows, piece, NT, preferred_element_type=f32).astype(bf16)
                for piece in pieces
            ],
            axis=1,
        )

    def to_own(parts):
        bit = n_tp // 2
        while bit:
            kept = []
            for at in range(bit):
                other = swap_tp(parts[at ^ bit], bit)
                kept.append(parts[at].astype(f32) + other.astype(f32))
            if bit > 1:
                kept = [k.astype(bf16) for k in kept]
            parts = kept
            bit //= 2
        return parts[0].astype(f32)

    def from_all(part):
        parts = [part]
        bit = 1
        while bit < n_tp:
            parts = parts + [swap_tp(p, bit) for p in parts]
            bit *= 2
        return parts

    mixer_parts = [
        project(mixed[slot * own_rows : (slot + 1) * own_rows], out_pieces)
        for slot in range(n_tp)
    ]
    mixer_sum = reorder(to_own(mixer_parts), order_o, order_m)
    after_mixer = (tokens_own.astype(f32) + mixer_sum).astype(bf16)
    normed_two = rms_rows(after_mixer, gain_m)

    total = after_mixer.astype(f32)
    back = []
    for mask in group:
        relabel = [m ^ mask for m in order_m]
        mine = normed_two if mask == 0 else swap(reorder(normed_two, order_m, relabel), mask)
        rows = jnp.concatenate(from_all(mine), axis=0)
        hidden = jnp.square(jax.nn.relu(fused_dot(rows, up_pieces))).astype(bf16)
        partial = project(hidden, down_pieces)
        reduced = to_own(
            [partial[slot * own_rows : (slot + 1) * own_rows] for slot in range(n_tp)]
        )
        if mask:
            returned = swap(reduced.astype(bf16), mask)
            back.append(reorder(returned, order_m, relabel).astype(f32))
        else:
            back.append(reduced)
    for term in back:
        total = total + term
    finished = from_all(total.astype(bf16))
    row_slots = jnp.concatenate(finished, axis=0).reshape(n_tp, own_rows, width)
    row_slots = row_slots[core ^ jnp.arange(n_tp)].reshape(length, width)
    places = [order_m.index(mask) for mask in range(n_fs)]
    return pick_columns(row_slots, jnp.array(places, jnp.int32)[me ^ jnp.arange(n_fs)])


def solution(mesh):
    return jax.shard_map(
        functools.partial(per_device, mesh.shape["fs"], mesh.shape["tp"]),
        mesh=mesh,
        in_specs=(
            P("fs", None),
            P(),
            P("fs", "tp"),
            P("fs", "tp"),
            P("fs", "tp"),
            P(),
            P(None, "tp"),
            P("tp"),
            P("fs", "tp"),
            P("tp"),
            P("fs", "tp"),
            P(),
            P("fs", "tp"),
            P("fs", "tp"),
        ),
        out_specs=P("fs", None),
        check_vma=False,
    )
```
